768 devices in a mesh: fs: 96 (over z, y), tp: 8 (over x, core).
Axes of the slice: x: 4, y: 8, z: 12, core: 2. Of those that a mesh axis runs over, the one named last changes fastest.
Arguments:
- inputs: bfloat16 [98304, 2304], P('fs'), may hold values from -20 to 20
- query_cot: bfloat16 [98304, 1024], P('fs', 'tp'), may hold values from -6 to 6
- head_out: bfloat16 [98304, 1024], P('fs', 'tp'), may hold values from -6 to 6
- out_cot: bfloat16 [98304, 2304], P('fs'), may hold values from -6 to 6
- query_factor: bfloat16 [2304, 192], P('fs'), may hold values from -2.5 to 2.5
- out_factor: bfloat16 [2304, 192], P('fs'), may hold values from -2.5 to 2.5
- query_master: float32 [2304, 1024], P('fs', 'tp'), may hold values from -0.125 to 0.125
- out_master: float32 [2304, 1024], P('fs', 'tp'), may hold values from -0.1875 to 0.1875
- query_first: float32 [192, 1024], P('fs', 'tp'), may hold values from -6 to 6
- query_second: float32 [192, 1024], P('fs', 'tp'), may hold values from 0.3 to 3
- out_first: float32 [192, 1024], P('fs', 'tp'), may hold values from -6 to 6
- out_second: float32 [192, 1024], P('fs', 'tp'), may hold values from 0.3 to 3
Outputs:
- query_step: float32 [2304, 1024], P('fs', 'tp')
- out_step: float32 [2304, 1024], P('fs', 'tp')
- query_copy: bfloat16 [2304, 1024], P(None, 'tp')
- out_copy: bfloat16 [2304, 1024], P(None, 'tp')
- query_first_new: float32 [192, 1024], P('fs', 'tp')
- query_second_new: float32 [192, 1024], P('fs', 'tp')
- out_first_new: float32 [192, 1024], P('fs', 'tp')
- out_second_new: float32 [192, 1024], P('fs', 'tp')
The draws below stay inside these ranges and needn't reach their ends.
All inputs are finite; a program needn't handle non-finite values.
Results may differ from the reference program's by a relative error of at most 0.0065.
Values may be sent and summed in bfloat16 or wider, within the bound.
No kernel may reach another device: no remote copies, remote signals or barrier semaphores. Data moves between devices by JAX's collectives and lax.ppermute only.
A program may use at most 64 MiB of HBM per device.

```python
import math
import jax
import jax.numpy as jnp
from jax import lax

D = 2304
RANK = 192
QC = 1024
TOKENS = 98304


def factor_table(key):
    base = jax.random.truncated_normal(jax.random.fold_in(key, 11), -4.0, 4.0, (D, RANK), jnp.float32)
    base = base * D ** (-0.5)
    rising = 3.0 ** (jnp.arange(RANK, dtype=jnp.float32) / RANK)
    rough = jnp.exp(jax.random.uniform(jax.random.fold_in(key, 12), (RANK,), jnp.float32, 0.0, math.log(3.3)))
    table = base * (rising * rough)[None, :]
    return table.astype(jnp.bfloat16)


def draw_query_factor(key, part):
    return factor_table(jax.random.fold_in(key, 1))


def draw_out_factor(key, part):
    return factor_table(jax.random.fold_in(key, 2))


def with_spikes(values, own_key, source, target, parts, factor):
    def block_of(axis_at):
        return (jnp.arange(values.shape[axis_at]) // (values.shape[axis_at] // parts)).reshape((-1,) + (1,) * (values.ndim - 1 - axis_at))

    first = jax.random.permutation(own_key, parts)[block_of(target)]
    second = (block_of(target) + parts // 2) % parts
    return jnp.where((block_of(source) == first) | (block_of(source) == second), factor * values, values)


def steps_of(rng, extent, shards, smallest, largest):
    def one(dim, blocks):
        draws = jax.random.uniform(jax.random.fold_in(jax.random.fold_in(rng, 6), dim), (blocks,), jnp.float32, smallest / len(shards), largest / len(shards))
        return jnp.repeat(jnp.exp(draws), extent[dim] // blocks).reshape((-1,) + (1,) * (len(extent) - dim - 1))

    level = one(*shards[0])
    for cut in shards[1:]:
        level = level * one(*cut)
    return level


def normal_values(rng, dims, spread, reach, shards=(), kind=jnp.bfloat16):
    gain = steps_of(rng, dims, shards, -0.22, 0.18) if shards else 1.0
    result = jax.random.normal(rng, dims, jnp.float32) * spread * gain
    return jnp.minimum(jnp.maximum(result, -reach), reach).astype(kind)


def heavy_noise(rng, extent, scale, limit, shards, heavy, kind=jnp.bfloat16):
    values = scale * jax.random.normal(rng, extent, jnp.float32)
    if shards:
        values = values * steps_of(rng, extent, shards, -0.22, 0.18)
    return jnp.clip(with_spikes(values, jax.random.fold_in(rng, 3), *heavy), -limit, limit).astype(kind)


def setup_inputs(seed: int = 0) -> dict:
    key_list = jax.random.split(jax.random.key(seed), 13)
    inputs = heavy_noise(key_list[0], (TOKENS, D), 1.0, 20.0, ((0, 96),), (0, 1, 96, 4.75))
    query_cot = normal_values(key_list[1], (TOKENS, QC), 1.0, 6.0, ((0, 96), (1, 8)))
    head_out = normal_values(key_list[2], (TOKENS, QC), 1.0, 6.0, ((0, 96), (1, 8)))
    out_cot = normal_values(key_list[3], (TOKENS, D), 1.0, 6.0, ((0, 96),))
    query_factor = draw_query_factor(jax.random.fold_in(key_list[12], 71), 0)
    out_factor = draw_out_factor(jax.random.fold_in(key_list[12], 71), 0)
    query_master = normal_values(key_list[6], (D, QC), D ** -0.5, 0.125, ((0, 96), (1, 8)), jnp.float32)
    out_master = normal_values(key_list[7], (D, QC), QC ** -0.5, 0.1875, ((0, 96), (1, 8)), jnp.float32)
    query_first = normal_values(key_list[8], (RANK, QC), 1.0, 6.0, ((0, 96), (1, 8)), jnp.float32)
    query_second = jnp.clip(jnp.exp(math.log(3.0) - 2.3025851 * jax.random.uniform(key_list[9], (RANK, QC), jnp.float32) ** steps_of(key_list[9], (RANK, QC), ((0, 96), (1, 8)), -0.2, 0.2)), 0.3, 3.0)
    out_first = normal_values(key_list[10], (RANK, QC), 1.0, 6.0, ((0, 96), (1, 8)), jnp.float32)
    out_second = jnp.clip(jnp.exp(math.log(3.0) - 2.3025851 * jax.random.uniform(key_list[11], (RANK, QC), jnp.float32) ** steps_of(key_list[11], (RANK, QC), ((0, 96), (1, 8)), -0.2, 0.2)), 0.3, 3.0)
    return dict(inputs=inputs, query_cot=query_cot, head_out=head_out, out_cot=out_cot, query_factor=query_factor, out_factor=out_factor, query_master=query_master, out_master=out_master, query_first=query_first, query_second=query_second, out_first=out_first, out_second=out_second)


beta_first = 0.8
beta_second = 0.95
adam_eps = 1e-08
learn_rate = 0.05
norm_eps = 1e-06

def moment_update(normed, first_old, second_old):
    first_new = beta_first * first_old + (1.0 - beta_first) * normed
    second_new = beta_second * second_old + (1.0 - beta_second) * normed * normed
    direction = (first_new / (jnp.sqrt(second_new) + adam_eps)).astype(jnp.bfloat16)
    return (first_new, second_new, direction)

def reference(inputs, query_cot, head_out, out_cot, query_factor, out_factor, query_master, out_master, query_first, query_second, out_first, out_second):
    grad_query = jnp.dot(inputs.T, query_cot, preferred_element_type=jnp.float32)
    proj_query = jnp.dot(query_factor.astype(jnp.float32).T, grad_query, precision=lax.Precision.HIGHEST)
    cot_low = jnp.dot(out_cot, out_factor, preferred_element_type=jnp.float32).astype(jnp.bfloat16)
    proj_out = jnp.dot(cot_low.T, head_out, preferred_element_type=jnp.float32)
    squares = jnp.sum(proj_query * proj_query) + jnp.sum(proj_out * proj_out)
    rms_value = jnp.sqrt(squares / (2.0 * RANK * QC) + norm_eps)
    first_q, second_q, dir_query = moment_update(proj_query / rms_value, query_first, query_second)
    first_o, second_o, dir_out = moment_update(proj_out / rms_value, out_first, out_second)
    query_step = jnp.dot(query_factor, dir_query, preferred_element_type=jnp.float32)
    out_step = jnp.dot(out_factor, dir_out, preferred_element_type=jnp.float32)
    query_copy = (query_master - learn_rate * query_step).astype(jnp.bfloat16)
    out_copy = (out_master - learn_rate * out_step).astype(jnp.bfloat16)
    return (query_step, out_step, query_copy, out_copy, first_q, second_q, first_o, second_o)
```

```python
import jax
import jax.numpy as jnp
from jax import lax
from jax.sharding import Mesh
from jax.sharding import PartitionSpec as P
from jax.experimental import pallas as pl
from jax.experimental.pallas import tpu as pltpu


RANK = 192
NZ, NY = 12, 8
FS = ("fs_0", "fs_1")
Z, Y, TP = "fs_0", "fs_1", "tp"

beta_first = 0.8
beta_second = 0.95
adam_eps = 1e-08
learn_rate = 0.05
norm_eps = 1e-06
contract_rows = (((0,), (0,)), ((), ()))
bf16 = jnp.bfloat16
f32 = jnp.float32


def spread(value, axis):
    peers = lax.axis_size(axis)
    return lax.all_to_all(
        jnp.broadcast_to(value[None], (peers, *value.shape)), axis, 0, 0, tiled=True
    )


def two_words(value):
    high = lax.reduce_precision(value, 8, 7)
    return high.astype(bf16), (value - high).astype(bf16)


def moment_update(normed, first_old, second_old):
    first_new = beta_first * first_old + (1.0 - beta_first) * normed
    second_new = beta_second * second_old + (1.0 - beta_second) * normed * normed
    direction = (first_new / (jnp.sqrt(second_new) + adam_eps)).astype(bf16)
    return (first_new, second_new, direction)


def own_first(rank_rows, nz, ny):
    place = jnp.arange(RANK)
    own_rows = rank_rows
    y, z, r = place // (nz * own_rows), (place // own_rows) % nz, place % own_rows
    source = (z * ny + y) * own_rows + r
    return (jnp.arange(RANK)[:, None] == source[None, :]).astype(bf16)


def assemble(own_piece, piece_1, piece_2, piece_3, other):
    pieces = (own_piece, piece_1, piece_2, piece_3)
    nz, rows, cols = own_piece.shape
    half = len(pieces)

    def kernel(*refs):
        mine, (other_ref, out_ref, sems) = refs[:half], refs[half:]
        tp = lax.axis_index(TP)
        x, core = tp // 2, tp % 2
        copies = []
        for k in range(half):
            slot = 2 * ((x + half - k) % half)
            copies.append(
                pltpu.make_async_copy(mine[k], out_ref.at[:, slot + core], sems.at[0, k])
            )
            copies.append(
                pltpu.make_async_copy(other_ref.at[k], out_ref.at[:, slot + 1 - core], sems.at[1, k])
            )
        for copy in copies:
            copy.start()
        for copy in copies:
            copy.wait()

    return pl.pallas_call(
        kernel,
        in_specs=[pl.BlockSpec(memory_space=pltpu.VMEM)] * (half + 1),
        out_specs=pl.BlockSpec(memory_space=pltpu.VMEM),
        scratch_shapes=[pltpu.SemaphoreType.DMA((2, half))],
        out_shape=jax.ShapeDtypeStruct((nz, 2 * half, rows, cols), bf16),
    )(*pieces, other)


def projected(inputs, out_cot, query_cot, head_out, factors, ny):
    tokens, model = inputs.shape
    columns = query_cot.shape[1]
    step = tokens // 4
    rows = RANK // ny

    def kernel(x_ref, o_ref, cot_ref, head_ref, f_ref, out_ref, acc_q, acc_o):
        at = pl.program_id(0)

        @pl.when(at == 0)
        def _():
            acc_q[...] = jnp.zeros_like(acc_q)
            acc_o[...] = jnp.zeros_like(acc_o)

        low = jnp.dot(x_ref[...], f_ref[:, :256], preferred_element_type=f32)
        high = low.astype(bf16)
        rest = (low - high.astype(f32)).astype(bf16)
        cot = cot_ref[...]
        acc_q[...] += lax.dot_general(
            high, cot, contract_rows, preferred_element_type=f32
        ) + lax.dot_general(rest, cot, contract_rows, preferred_element_type=f32)
        low = jnp.dot(o_ref[...], f_ref[:, 128:], preferred_element_type=f32).astype(bf16)
        acc_o[...] += lax.dot_general(low, head_ref[...], contract_rows, preferred_element_type=f32)

        @pl.when(at == pl.num_programs(0) - 1)
        def _():
            for y in range(ny):
                out_ref[y, :rows] = acc_q[y * rows : (y + 1) * rows]
                out_ref[y, rows:] = acc_o[64 + y * rows : 64 + (y + 1) * rows]

    return pl.pallas_call(
        kernel,
        grid=(tokens // step,),
        in_specs=[
            pl.BlockSpec((step, model), lambda i: (i, 0)),
            pl.BlockSpec((step, model), lambda i: (i, 0)),
            pl.BlockSpec((step, columns), lambda i: (i, 0)),
            pl.BlockSpec((step, columns), lambda i: (i, 0)),
            pl.BlockSpec((model, 2 * RANK), lambda i: (0, 0)),
        ],
        out_specs=pl.BlockSpec((ny, 2 * rows, columns), lambda i: (0, 0, 0)),
        out_shape=jax.ShapeDtypeStruct((ny, 2 * rows, columns), f32),
        scratch_shapes=[pltpu.VMEM((256, columns), f32), pltpu.VMEM((256, columns), f32)],
    )(inputs, out_cot, query_cot, head_out, factors)


def update(
    inputs,
    query_cot,
    head_out,
    out_cot,
    query_factor,
    out_factor,
    query_master,
    out_master,
    query_first,
    query_second,
    out_first,
    out_second,
):
    own = query_factor.shape[0]
    own_rows = query_first.shape[0]
    nz, ny, peers = lax.axis_size(Z), lax.axis_size(Y), lax.axis_size(TP)
    order = own_first(own_rows, nz, ny)
    factor_q = jnp.dot(query_factor, order, preferred_element_type=f32).astype(bf16)
    factor_o = jnp.dot(out_factor, order, preferred_element_type=f32).astype(bf16)
    shard = lax.ppermute(
        jnp.concatenate([factor_q, factor_o], axis=1),
        (Y, TP),
        [(i * ny + j, j * ny + i) for i in range(ny) for j in range(ny)],
    )
    moments = jnp.concatenate([query_first, query_second, out_first, out_second], axis=0)
    moments = jnp.concatenate(two_words(moments), axis=0)
    moments = jnp.pad(moments, ((0, own - moments.shape[0]), (0, 0)))
    late = [query_master.astype(bf16), out_master.astype(bf16), moments]
    over_z = spread(jnp.concatenate([shard, *late], axis=1), Z)
    masters = spread(over_z[:, :, 384:640], Y)
    piece = over_z[:, :, :384]
    along = [piece]
    for k in range(1, peers // 2):
        moves = [(i, (i + 2 * k) % peers) for i in range(peers)]
        along.append(lax.ppermute(piece, TP, moves))
    other = lax.ppermute(jnp.stack(along), TP, [(i, i ^ 1) for i in range(peers)])
    factors = assemble(*along, other).reshape(nz * ny * own, 2 * RANK)

    terms = projected(inputs, out_cot, query_cot, head_out, factors, ny)
    terms, masters = lax.optimization_barrier((terms, masters))

    split = lax.all_to_all(terms, Y, 0, 0, tiled=True)
    whole = spread(split.sum(axis=0), Z).sum(axis=0)
    sq_total = spread(jnp.sum(whole * whole)[None, None], (Y, TP)).sum()
    count_all = 2.0 * RANK * terms.shape[-1] * peers
    rms_value = jnp.sqrt(sq_total / count_all + norm_eps)
    normed = (whole / rms_value).reshape(2, nz * own_rows, -1)
    words = over_z[:, : 8 * own_rows, 640:].astype(f32).reshape(nz, 2, 4, own_rows, -1)
    old = (words[:, 0] + words[:, 1]).transpose(1, 0, 2, 3).reshape(4, nz * own_rows, -1)
    first_q, second_q, dir_q = moment_update(normed[0], old[0], old[1])
    first_o, second_o, dir_o = moment_update(normed[1], old[2], old[3])
    dirs = spread(jnp.concatenate([dir_q, dir_o], axis=0), Y)
    half = nz * own_rows
    dir_q = dirs[:, :half].reshape(RANK, -1)
    dir_o = dirs[:, half:].reshape(RANK, -1)

    masters = masters.transpose(1, 0, 2, 3).reshape(nz * ny * own, -1)
    columns = query_master.shape[1]
    full_q = jnp.dot(factors[:, :RANK], dir_q, preferred_element_type=f32)
    full_o = jnp.dot(factors[:, RANK:], dir_o, preferred_element_type=f32)
    query_copy = (masters[:, :columns].astype(f32) - learn_rate * full_q).astype(bf16)
    out_copy = (masters[:, columns:].astype(f32) - learn_rate * full_o).astype(bf16)
    query_step = jnp.dot(factor_q, dir_q, preferred_element_type=f32)
    out_step = jnp.dot(factor_o, dir_o, preferred_element_type=f32)

    row = lax.axis_index(Z) * own_rows
    own_q = lax.dynamic_slice_in_dim(normed[0], row, own_rows, 0)
    own_o = lax.dynamic_slice_in_dim(normed[1], row, own_rows, 0)
    first_q, second_q, _ = moment_update(own_q, query_first, query_second)
    first_o, second_o, _ = moment_update(own_o, out_first, out_second)
    return (query_step, out_step, query_copy, out_copy, first_q, second_q, first_o, second_o)


def solution(mesh):
    torus = Mesh(mesh.devices.reshape(NZ, NY, mesh.shape["tp"]), ("fs_0", "fs_1", "tp"))
    placed = (
        P(FS, None),
        P(FS, "tp"),
        P(FS, "tp"),
        P(FS, None),
        P(FS, None),
        P(FS, None),
        P(FS, "tp"),
        P(FS, "tp"),
        P(FS, "tp"),
        P(FS, "tp"),
        P(FS, "tp"),
        P(FS, "tp"),
    )
    return jax.shard_map(
        update,
        mesh=torus,
        in_specs=placed,
        out_specs=(
            P(FS, "tp"),
            P(FS, "tp"),
            P(None, "tp"),
            P(None, "tp"),
            P(FS, "tp"),
            P(FS, "tp"),
            P(FS, "tp"),
            P(FS, "tp"),
        ),
        check_vma=False,
    )
```
